32 devices in a mesh: sp: 16 (over z, y, core), tp: 2 (over x).
Axes of the slice: x: 2, y: 2, z: 4, core: 2. Of those that a mesh axis runs over, the one named last changes fastest.
Arguments:
- queries: bfloat16 [16384, 1024], P('sp', 'tp'), may hold values from -8 to 8
- keyvals: bfloat16 [16384, 8, 128], P('sp', 'tp'), may hold values from -8 to 8
- head_sink_logit: float32 [16], P('tp'), may hold values from 2 to 7
- doc_ids: int32 [16384], P('sp'), may hold values from 0 to 7, never falling along the last dimension, each value on 1 to 4096 neighbouring positions
- stream_in: bfloat16 [16384, 2048], P(('sp', 'tp')), may hold values from -6 to 6
- out_weight: bfloat16 [1024, 2048], replicated, may hold values from -1.5 to 1.5
- first_gain: float32 [2048], replicated, may hold values from 0.1 to 1.9
- up_weight: bfloat16 [2048, 8192], P('sp', 'tp'), may hold values from -0.125 to 0.125
- down_weight: bfloat16 [8192, 2048], P('tp', 'sp'), may hold values from -0.0625 to 0.0625
- second_gain: float32 [2048], replicated, may hold values from 0.1 to 1.9
Outputs:
- layer_out: bfloat16 [16384, 2048], P(('sp', 'tp'))
The draws below stay inside these ranges and needn't reach their ends.
Inputs may be any that keep to these rules, and one draw needn't show every extreme that they name: `doc_ids`: document numbers never fall along the sequence.
All inputs are finite; a program needn't handle non-finite values.
Results may differ from the reference program's by a relative error of at most 0.013.
Values may be sent and summed in bfloat16 or wider, within the bound.
No kernel may reach another device: no remote copies, remote signals or barrier semaphores. Data moves between devices by JAX's collectives and lax.ppermute only.
A program may use at most 128 MiB of HBM per device.

```python
import math
import jax
import jax.numpy as jnp
import numpy as np
from jax import lax

D = 2048
FF = 8192
QUERY_HEADS = 16
KEY_VALUE_HEADS = 8
HEAD_SIZE = 64
WINDOW_REACH = 128
PACKED_TOKENS = 16384
N_SP = 16
N_TP = 2


def draw_queries(key, part):
    self_key = jax.random.fold_in(key, 3)
    value_rows = jnp.clip(jax.random.normal(self_key, (PACKED_TOKENS, QUERY_HEADS, HEAD_SIZE), jnp.float32), -6.0, 6.0)
    return value_rows.reshape(PACKED_TOKENS, QUERY_HEADS * HEAD_SIZE).astype(jnp.bfloat16)


def draw_keyvals(key, part):
    self_key = jax.random.fold_in(key, 5)
    value_rows = jnp.clip(jax.random.normal(self_key, (PACKED_TOKENS, KEY_VALUE_HEADS, 2 * HEAD_SIZE), jnp.float32), -6.0, 6.0)
    return value_rows.astype(jnp.bfloat16)


def levels(stream_key, shape, cuts, smallest, high):
    def one(position, shards_of):
        steps = jax.random.uniform(jax.random.fold_in(jax.random.fold_in(stream_key, 6), position), (shards_of,), jnp.float32, smallest / len(cuts), high / len(cuts))
        return jnp.repeat(jnp.exp(steps), shape[position] // shards_of).reshape((-1,) + (1,) * (len(shape) - position - 1))

    level = one(*cuts[0])
    for cut in cuts[1:]:
        level = level * one(*cut)
    return level


def profile(number_of, total, most, slope):
    weights = [(1 << 20) // math.isqrt(grade ** slope) + 1 for grade in range(2, number_of + 1)]
    spare, given = total - most - (number_of - 1), [1] * (number_of - 1)
    while spare > 0:
        movable = [i for i in range(number_of - 1) if given[i] < most]
        pool, remaining = sum([weights[i] for i in movable]), spare
        for i in movable:
            extra = min(most - given[i], max(1, remaining * weights[i] // pool), spare)
            given[i] = given[i] + extra
            spare = spare - extra
    return np.array([most] + given)


def uneven(rng, count, total, most, skew):
    if count == 2:
        one = jax.random.randint(rng, (), max(1, total - most), min(most, total - 1) + 1)
        return jnp.stack([one, total - one])
    lengths = jnp.asarray(profile(count, total, most, skew), jnp.int32)
    couples = (count - 1) // 2
    source_of, sink = lengths[1:1 + 2 * couples:2], lengths[2:2 + 2 * couples:2]
    margin = jnp.minimum(source_of - 1, most - sink)
    passed = jax.random.randint(jax.random.fold_in(rng, 1), (couples,), 0, 1 << 20) % (margin + 1)
    lengths = lengths.at[1:1 + 2 * couples:2].set(source_of - passed).at[2:2 + 2 * couples:2].set(sink + passed)
    return lengths[jax.random.permutation(jax.random.fold_in(rng, 2), count)]


def noise(stream_key, shape, scale, most, shards=(), kind=jnp.bfloat16):
    array = jax.random.normal(stream_key, shape, jnp.float32) * scale
    if len(shards) > 0:
        array = levels(stream_key, shape, shards, -0.22, 0.18) * array
    return jnp.clip(array, min=-most, max=most).astype(kind)


def setup_inputs(seed: int = 0) -> dict:
    seeds = jax.random.split(jax.random.key(seed), 11)
    queries = draw_queries(jax.random.fold_in(seeds[10], 71), 0)
    keyvals = draw_keyvals(jax.random.fold_in(seeds[10], 71), 0)
    head_sink_logit = jnp.clip(2.0 + 5.0 * jax.random.uniform(seeds[2], (QUERY_HEADS,), jnp.float32) ** levels(seeds[2], (QUERY_HEADS,), ((0, 2),), -0.2, 0.2), 2.0, 7.0)
    doc_ids = jnp.searchsorted(jnp.cumsum(uneven(seeds[3], N_SP // 2, PACKED_TOKENS, PACKED_TOKENS // 4, 1)), jnp.arange(PACKED_TOKENS), side="right").astype(jnp.int32)
    stream_in = noise(seeds[4], (PACKED_TOKENS, D), 1.0, 6.0, ((0, 32),))
    out_weight = noise(seeds[5], (QUERY_HEADS * HEAD_SIZE, D), (QUERY_HEADS * HEAD_SIZE // 64) ** -0.5, 1.5)
    first_gain = jnp.clip(1.0 + 0.18 * jax.random.normal(seeds[6], (D,), jnp.float32), 0.1, 1.9)
    up_weight = noise(seeds[7], (D, FF), D ** -0.5, 0.125, ((0, 16), (1, 2)))
    down_weight = noise(seeds[8], (FF, D), FF ** -0.5, 0.0625, ((0, 2), (1, 16)))
    second_gain = jnp.clip(1.0 + 0.18 * jax.random.normal(seeds[9], (D,), jnp.float32), 0.1, 1.9)
    return dict(queries=queries, keyvals=keyvals, head_sink_logit=head_sink_logit, doc_ids=doc_ids, stream_in=stream_in, out_weight=out_weight, first_gain=first_gain, up_weight=up_weight, down_weight=down_weight, second_gain=second_gain)


NEG_LARGE = -1e+30
NORM_EPS = 1e-05

def layer_norm(stream, gain_row):
    centre = lax.optimization_barrier(jnp.mean(stream, axis=-1, keepdims=True))
    shifted = stream - centre
    spread = lax.optimization_barrier(jnp.mean(shifted * shifted, axis=-1, keepdims=True))
    return shifted * lax.rsqrt(spread + NORM_EPS) * gain_row

def window_attention(queries, keyvals, head_sink_logit, doc_ids):
    block_list = PACKED_TOKENS // WINDOW_REACH
    heads_per_group = QUERY_HEADS // KEY_VALUE_HEADS
    score_scale = HEAD_SIZE ** (-0.5)
    query_block_list = queries.astype(jnp.float32).reshape(block_list, WINDOW_REACH, KEY_VALUE_HEADS, heads_per_group, HEAD_SIZE).transpose(2, 0, 1, 3, 4)
    padding_width = jnp.zeros((WINDOW_REACH, KEY_VALUE_HEADS, 2 * HEAD_SIZE), jnp.float32)
    padded_rows = jnp.concatenate([padding_width, keyvals.astype(jnp.float32), padding_width], axis=0).reshape(block_list + 2, WINDOW_REACH, KEY_VALUE_HEADS, 2 * HEAD_SIZE)
    banded = jnp.concatenate([padded_rows[:-2], padded_rows[1:-1], padded_rows[2:]], axis=1).transpose(2, 0, 1, 3)
    doc_pad = jnp.zeros((WINDOW_REACH,), jnp.int32)
    doc_ext = jnp.concatenate([doc_pad, doc_ids, doc_pad]).reshape(block_list + 2, WINDOW_REACH)
    doc_band = jnp.concatenate([doc_ext[:-2], doc_ext[1:-1], doc_ext[2:]], axis=1)
    query_pos = jnp.arange(PACKED_TOKENS, dtype=jnp.int32).reshape(block_list, WINDOW_REACH, 1)
    key_pos = (jnp.arange(block_list, dtype=jnp.int32)[:, None] * WINDOW_REACH + jnp.arange(3 * WINDOW_REACH, dtype=jnp.int32)[None, :] - WINDOW_REACH)[:, None, :]
    allowed = (jnp.abs(query_pos - key_pos) <= WINDOW_REACH) & (key_pos >= 0) & (key_pos < PACKED_TOKENS) & (doc_ids.reshape(block_list, WINDOW_REACH, 1) == doc_band[:, None, :])
    sink_logit_table = head_sink_logit.reshape(KEY_VALUE_HEADS, heads_per_group)

    def one_head(operands):
        query_head, band_head, sink_head = operands
        scores = jnp.einsum('nqgd,nkd->ngqk', query_head, band_head[..., :HEAD_SIZE]) * score_scale
        scores = jnp.where(allowed[:, None], scores, NEG_LARGE)
        sink_col = sink_head[None, :, None, None]
        highest = jnp.maximum(lax.optimization_barrier(jnp.max(scores, axis=-1, keepdims=True)), sink_col)
        powers = jnp.exp(scores - highest)
        denominator = lax.optimization_barrier(jnp.sum(powers, axis=-1, keepdims=True)) + jnp.exp(sink_col - highest)
        weights = lax.optimization_barrier((powers / denominator).astype(jnp.bfloat16)).astype(jnp.float32)
        mixed_out = jnp.einsum('ngqk,nkd->nqgd', weights, band_head[..., HEAD_SIZE:])
        return mixed_out.astype(jnp.bfloat16)
    heads_out = lax.map(one_head, (query_block_list, banded, sink_logit_table))
    return heads_out.transpose(1, 2, 0, 3, 4).reshape(PACKED_TOKENS, QUERY_HEADS * HEAD_SIZE)

def reference(queries, keyvals, head_sink_logit, doc_ids, stream_in, out_weight, first_gain, up_weight, down_weight, second_gain):
    attended = window_attention(queries, keyvals, head_sink_logit, doc_ids)
    projected = jnp.dot(attended, out_weight, preferred_element_type=jnp.float32)
    first_stream = layer_norm(stream_in.astype(jnp.float32) + projected, first_gain).astype(jnp.bfloat16)
    ff_share = FF // N_TP
    up_groups = up_weight.reshape(D, N_TP, ff_share).transpose(1, 0, 2)
    down_groups = down_weight.reshape(N_TP, ff_share, D)

    def add_group(running, weight_pair):
        up_part, down_part = weight_pair
        hidden = jnp.dot(first_stream, up_part, preferred_element_type=jnp.float32)
        active = jnp.square(jnp.maximum(hidden, 0.0)).astype(jnp.bfloat16)
        partial_value = jnp.dot(active, down_part, preferred_element_type=jnp.float32)
        rounded = lax.optimization_barrier(partial_value.astype(jnp.bfloat16)).astype(jnp.float32)
        return (running + rounded, None)
    mixed_out, unused_out = lax.scan(add_group, jnp.zeros((PACKED_TOKENS, D), jnp.float32), (up_groups, down_groups))
    return layer_norm(first_stream.astype(jnp.float32) + mixed_out, second_gain).astype(jnp.bfloat16)
```

```python
import functools

import jax
import jax.numpy as jnp
from jax import lax
from jax.experimental import pallas as pl
from jax.experimental.pallas import tpu as pltpu
from jax.sharding import PartitionSpec as P

HEAD_SIZE = 64
WINDOW_REACH = 128


NEG_LARGE = -1e30
NORM_EPS = 1e-05


def padded(block, sides, width):
    for axis, dim in sides:
        count = lax.axis_size(axis)
        forward = [(i, i + 1) for i in range(count - 1)]
        backward = [(target, source) for source, target in forward]
        low = lax.ppermute(
            lax.slice_in_dim(block, block.shape[dim] - width, None, axis=dim), axis, forward
        )
        high = lax.ppermute(lax.slice_in_dim(block, 0, width, axis=dim), axis, backward)
        block = jnp.concatenate([low, block, high], axis=dim)
    return block


def layer_norm(stream, gain_row):
    centre = jnp.mean(stream, axis=-1, keepdims=True)
    shifted = stream - centre
    spread = jnp.mean(shifted * shifted, axis=-1, keepdims=True)
    return shifted * lax.rsqrt(spread + NORM_EPS) * gain_row


def attend(queries, keyvals, head_sink_logit, doc_ids):
    tok_rows = queries.shape[0]
    kv_heads = keyvals.shape[1]
    heads_per_group = queries.shape[1] // (HEAD_SIZE * kv_heads)
    block_list = tok_rows // WINDOW_REACH
    score_scale = HEAD_SIZE ** (-0.5)
    doc_marks = doc_ids.astype(jnp.bfloat16)
    rim_keys, rim_docs = (
        padded(keyvals, (("sp", 0),), WINDOW_REACH),
        padded(doc_marks, (("sp", 0),), WINDOW_REACH),
    )
    padded_rows = rim_keys.reshape(block_list + 2, WINDOW_REACH, kv_heads, 2 * HEAD_SIZE)
    banded = jnp.concatenate([padded_rows[:-2], padded_rows[1:-1], padded_rows[2:]], axis=1)
    doc_ext = rim_docs.reshape(block_list + 2, WINDOW_REACH)
    doc_band = jnp.concatenate([doc_ext[:-2], doc_ext[1:-1], doc_ext[2:]], axis=1)
    offset = lax.axis_index("sp") * tok_rows
    total_rows = tok_rows * lax.axis_size("sp")
    query_pos = offset + jnp.arange(tok_rows, dtype=jnp.int32).reshape(block_list, WINDOW_REACH, 1)
    key_pos = (
        offset
        + (
            jnp.arange(block_list, dtype=jnp.int32)[:, None] * WINDOW_REACH
            + jnp.arange(3 * WINDOW_REACH, dtype=jnp.int32)[None, :]
            - WINDOW_REACH
        )[:, None, :]
    )
    allowed = (
        (jnp.abs(query_pos - key_pos) <= WINDOW_REACH)
        & (key_pos >= 0)
        & (key_pos < total_rows)
        & (doc_marks.reshape(block_list, WINDOW_REACH, 1) == doc_band[:, None, :])
    )
    query_block_list = queries.reshape(
        block_list, WINDOW_REACH, kv_heads, heads_per_group, HEAD_SIZE
    )
    scores = (
        jnp.einsum(
            "nqhgd,nkhd->nhgqk",
            query_block_list,
            banded[..., :HEAD_SIZE],
            preferred_element_type=jnp.float32,
        )
        * score_scale
    )
    scores = jnp.where(allowed[:, None, None], scores, NEG_LARGE)
    sink_col = head_sink_logit.reshape(kv_heads, heads_per_group)[None, :, :, None, None]
    highest = jnp.maximum(jnp.max(scores, axis=-1, keepdims=True), sink_col)
    powers = jnp.exp(scores - highest)
    denominator = jnp.sum(powers, axis=-1, keepdims=True) + jnp.exp(sink_col - highest)
    weights = (powers / denominator).astype(jnp.bfloat16)
    mixed_out = jnp.einsum(
        "nhgqk,nkhd->nqhgd", weights, banded[..., HEAD_SIZE:], preferred_element_type=jnp.float32
    )
    return mixed_out.astype(jnp.bfloat16).reshape(tok_rows, kv_heads * heads_per_group * HEAD_SIZE)


def per_device(
    queries,
    keyvals,
    head_sink_logit,
    doc_ids,
    stream_in,
    out_weight,
    first_gain,
    up_weight,
    down_weight,
    second_gain,
):
    up_whole = lax.all_gather(up_weight, "sp", axis=0, tiled=True)
    down_whole = lax.all_gather(down_weight, "sp", axis=1, tiled=True)
    attended = attend(queries, keyvals, head_sink_logit, doc_ids)
    tp_count = lax.axis_size("tp")
    own_rows = attended.shape[0] // tp_count
    by_peer = attended.reshape(tp_count, own_rows, attended.shape[1])
    projected = jnp.dot(
        lax.all_to_all(by_peer, "tp", split_axis=0, concat_axis=2, tiled=True)[0],
        out_weight,
        preferred_element_type=jnp.float32,
    )[None][0]
    first_stream = layer_norm(stream_in.astype(jnp.float32) + projected, first_gain).astype(
        jnp.bfloat16
    )
    hidden = jnp.dot(
        lax.all_gather(first_stream, "tp", axis=0, tiled=True),
        up_whole,
        preferred_element_type=jnp.float32,
    )
    active = jnp.square(jnp.maximum(hidden, 0.0)).astype(jnp.bfloat16)
    mixed_out = lax.psum_scatter(
        jnp.dot(active, down_whole, preferred_element_type=jnp.float32).astype(jnp.bfloat16),
        "tp",
        scatter_dimension=0,
        tiled=True,
    ).astype(jnp.float32)
    return layer_norm(first_stream.astype(jnp.float32) + mixed_out, second_gain).astype(
        jnp.bfloat16
    )


def attend_body(kv_heads, total_rows, place, sinks, query, low, own, high, out, band, held, probs):
    reach = WINDOW_REACH
    tok_rows = own.shape[0]
    unit = 2 * HEAD_SIZE
    step = pl.program_id(0)
    block = place[0] + step

    @pl.when(step == 0)
    def _():
        band[:reach] = low[...]
        band[reach : reach + tok_rows] = own[...]
        band[reach + tok_rows :] = high[...]

    start = pl.multiple_of(block * reach, reach)
    marks = slice(kv_heads * unit, (kv_heads + 1) * unit)
    key_docs = band[pl.ds(start, 3 * reach), marks].astype(jnp.float32).T
    query_docs = band[pl.ds(start + reach, reach), marks].astype(jnp.float32)
    shape = (reach, 3 * reach)
    row = lax.broadcasted_iota(jnp.int32, shape, 0)
    column = lax.broadcasted_iota(jnp.int32, shape, 1) - reach
    key_pos = place[1] + start + column
    allowed = (
        (jnp.abs(row - column) <= reach)
        & (key_pos >= 0)
        & (key_pos < total_rows)
        & (key_docs[:reach] == jnp.concatenate([query_docs] * 3, axis=1))
    )
    key_lanes = lax.broadcasted_iota(jnp.int32, (2 * reach, unit), 1) < HEAD_SIZE
    scale = jnp.array(HEAD_SIZE**-0.5, query.dtype)
    for head in range(kv_heads):
        pair = band[pl.ds(start, 3 * reach), head * unit : (head + 1) * unit]
        first = query[:, head * unit : (head + 1) * unit] * scale
        second = jnp.concatenate([first[:, HEAD_SIZE:], first[:, :HEAD_SIZE]], axis=1)
        both = jnp.concatenate([first, second], axis=0)
        both = jnp.where(key_lanes, both, jnp.zeros_like(both))
        scores = lax.dot_general(
            both, pair, (((1,), (1,)), ((), ())), preferred_element_type=jnp.float32
        )
        for member in range(2):
            part = scores[member * reach : (member + 1) * reach]
            held[2 * head + member] = jnp.where(allowed, part, NEG_LARGE)
    for number in range(2 * kv_heads):
        scores = held[number]
        sink = sinks[number]
        highest = jnp.maximum(jnp.max(scores, axis=-1, keepdims=True), sink)
        powers = jnp.exp(scores - highest)
        denominator = jnp.sum(powers, axis=-1, keepdims=True) + jnp.exp(sink - highest)
        at = slice((number % 2) * reach, (number % 2 + 1) * reach)
        probs[number // 2, at] = (powers * (1.0 / denominator)).astype(probs.dtype)
    for head in range(kv_heads):
        pair = band[pl.ds(start, 3 * reach), head * unit : (head + 1) * unit]
        mixed = jnp.dot(probs[head], pair, preferred_element_type=jnp.float32)
        first = pltpu.roll(mixed[:reach], HEAD_SIZE, 1)
        joined = jnp.where(key_lanes[:reach], first, mixed[reach:])
        out[:, head * unit : (head + 1) * unit] = joined.astype(out.dtype)


def attend_rows(kv_heads, total_rows, place, sinks, queries, low, own, high, rows):
    reach = WINDOW_REACH
    width = queries.shape[1]
    whole = lambda array: pl.BlockSpec(array.shape, lambda n, place, sinks: (0, 0))
    return pl.pallas_call(
        functools.partial(attend_body, kv_heads, total_rows),
        grid_spec=pltpu.PrefetchScalarGridSpec(
            num_scalar_prefetch=2,
            grid=(rows // reach,),
            in_specs=[
                pl.BlockSpec((reach, width), lambda n, place, sinks: (place[0] + n, 0)),
                whole(low),
                whole(own),
                whole(high),
            ],
            out_specs=pl.BlockSpec((reach, width), lambda n, place, sinks: (n, 0)),
            scratch_shapes=[
                pltpu.VMEM((own.shape[0] + 2 * reach, own.shape[1]), own.dtype),
                pltpu.VMEM((2 * kv_heads, reach, 3 * reach), jnp.float32),
                pltpu.VMEM((kv_heads, 2 * reach, 3 * reach), own.dtype),
            ],
        ),
        out_shape=jax.ShapeDtypeStruct((rows, width), queries.dtype),
        cost_estimate=pl.CostEstimate(
            flops=12 * rows * width * reach * 10, bytes_accessed=rows * width * 8, transcendentals=0
        ),
        name="attend_rows",
    )(place, sinks, queries, low, own, high)


def line_shape(mesh):
    devices = mesh.devices
    names = list(mesh.axis_names)
    if names != ["sp", "tp"]:
        return None
    count, tp_count = devices.shape
    where = [(*devices[i, 0].coords, devices[i, 0].core_on_chip) for i in range(count)]
    zs = sorted({w[2] for w in where})
    ys = sorted({w[1] for w in where})
    cores = sorted({w[3] for w in where})
    expected = [(where[0][0], y, z, c) for z in zs for y in ys for c in cores]
    if where != expected or tp_count != 2 or (len(zs), len(ys), len(cores)) != (4, 2, 2):
        return None
    return len(zs), len(ys), len(cores)


def up_body(tile, unit, order, *rest):
    count = order.shape[0]
    rows = rest[:4]
    weights = rest[4 : 4 + count]
    outs = rest[4 + count : 7 + count]
    buffer, sems = rest[7 + count :]
    step = pl.program_id(0)
    steps = pl.num_programs(0)

    def copies(index, slot):
        return [
            pltpu.make_async_copy(
                weight.at[:, pl.ds(pl.multiple_of(index * tile, tile), tile)],
                buffer.at[
                    slot, pl.ds(pl.multiple_of(order[j] * unit, unit), weight.shape[0]), :
                ],
                sems.at[slot, j],
            )
            for j, weight in enumerate(weights)
        ]

    slot = lax.rem(step, 2)

    @pl.when(step == 0)
    def _():
        for copy in copies(step, slot):
            copy.start()

    @pl.when(step + 1 < steps)
    def _():
        for copy in copies(step + 1, 1 - slot):
            copy.start()

    for copy in copies(step, slot):
        copy.wait()
    size = rows[0].shape[0]
    places = ((outs[0], 0), (outs[0], size), (outs[1], 0), (outs[2], 0))
    for part, (out, first) in zip(rows, places):
        hidden = jnp.dot(part[...], buffer[slot], preferred_element_type=jnp.float32)
        out[first : first + size] = jnp.square(jnp.maximum(hidden, 0.0)).astype(out.dtype)


def up_project(order, rows, weights):
    hidden_units = weights[0].shape[1]
    unit = min(weight.shape[0] for weight in weights)
    tile = min(512, hidden_units)
    count, width = rows[0].shape
    dtype = rows[0].dtype
    return pl.pallas_call(
        functools.partial(up_body, tile, unit),
        grid_spec=pltpu.PrefetchScalarGridSpec(
            num_scalar_prefetch=1,
            grid=(hidden_units // tile,),
            in_specs=[pl.BlockSpec((count, width), lambda n, order: (0, 0))] * 4
            + [pl.BlockSpec(memory_space=pl.ANY)] * len(weights),
            out_specs=[
                pl.BlockSpec((size, tile), lambda n, order: (0, n))
                for size in (2 * count, count, count)
            ],
            scratch_shapes=[
                pltpu.VMEM((2, width, tile), dtype),
                pltpu.SemaphoreType.DMA((2, len(weights))),
            ],
        ),
        out_shape=[
            jax.ShapeDtypeStruct((size, hidden_units), dtype) for size in (2 * count, count, count)
        ],
        cost_estimate=pl.CostEstimate(
            flops=8 * count * width * hidden_units,
            bytes_accessed=2 * width * hidden_units,
            transcendentals=0,
        ),
        name="up_project",
    )(order, *rows, *weights)


def norm_body(parts, order, stream, gain, *rest):
    mine = rest[:parts]
    theirs = rest[parts : 2 * parts]
    out, total = rest[2 * parts :]
    block = 0
    width = total.shape[1]
    unit = width // order.shape[0]
    for own, other in zip(mine, theirs):
        for j in range(own.shape[1] // unit):
            at = pl.ds(pl.multiple_of(order[block] * unit, unit), unit)
            piece = slice(j * unit, (j + 1) * unit)
            total[:, at] = own[:, piece].astype(jnp.float32) + other[:, piece].astype(jnp.float32)
            block += 1
    full = stream[...].astype(jnp.float32) + total[...]
    out[...] = layer_norm(full, gain[...]).astype(out.dtype)


def norm_sum(order, stream, gain, mine, theirs):
    rows, width = stream.shape
    tile = min(128, rows)
    part_specs = [
        pl.BlockSpec((tile, part.shape[1]), lambda n, order: (n, 0)) for part in [*mine, *theirs]
    ]
    return pl.pallas_call(
        functools.partial(norm_body, len(mine)),
        grid_spec=pltpu.PrefetchScalarGridSpec(
            num_scalar_prefetch=1,
            grid=(rows // tile,),
            in_specs=[
                pl.BlockSpec((tile, width), lambda n, order: (n, 0)),
                pl.BlockSpec((1, width), lambda n, order: (0, 0)),
                *part_specs,
            ],
            out_specs=pl.BlockSpec((tile, width), lambda n, order: (n, 0)),
            scratch_shapes=[pltpu.VMEM((tile, width), jnp.float32)],
        ),
        out_shape=jax.ShapeDtypeStruct((rows, width), stream.dtype),
        name="norm_sum",
    )(order, stream, gain.reshape(1, width), *mine, *theirs)


def per_device_line(
    shape,
    queries,
    keyvals,
    head_sink_logit,
    doc_ids,
    stream_in,
    out_weight,
    first_gain,
    up_weight,
    down_weight,
    second_gain,
):
    nz, ny, nc = shape

    def index(z, y, c):
        return (z * ny + y) * nc + c

    def pairs(target):
        found = []
        for z in range(nz):
            for y in range(ny):
                for c in range(nc):
                    to = target(z, y, c)
                    if to is not None:
                        found.append((index(z, y, c), index(*to)))
        return found

    ring = [(z, 0) for z in range(nz)] + [(z, 1) for z in reversed(range(nz))]
    chips = len(ring)

    def turned(by):
        return pairs(lambda z, y, c: (*ring[(ring.index((z, y)) + by) % chips], c))

    onward = turned(1)
    backward = turned(-1)
    twin = pairs(lambda z, y, c: (z, y, 1 - c))
    swap = [(0, 1), (1, 0)]

    me = lax.axis_index("sp")
    my_c = me % nc
    my_y = (me // nc) % ny
    my_z = me // (nc * ny)
    tp_me = lax.axis_index("tp")

    def send(value, way, axis="sp"):
        return lax.ppermute(value, axis, way)

    def halved(weight, hidden_axis):
        half = weight.shape[hidden_axis] // nc
        kept = lax.dynamic_slice_in_dim(weight, my_c * half, half, hidden_axis)
        given = lax.dynamic_slice_in_dim(weight, (1 - my_c) * half, half, hidden_axis)
        taken = send(given, twin)
        low = jnp.where(my_c == 0, kept, taken)
        high = jnp.where(my_c == 0, taken, kept)
        return jnp.concatenate([low, high], axis=1 - hidden_axis)

    def pass_on(left, right):
        return send(left, onward), send(right, backward)

    def half(block, number):
        rows = block.shape[0] // 2
        return lax.slice_in_dim(block, number * rows, (number + 1) * rows, axis=0)

    up_own = halved(up_weight, 1)
    up_blocks = [up_own]
    left = right = up_own
    for step in range(1, chips // 2):
        left, right = pass_on(left, right)
        up_blocks += [left, right]
    up_blocks += pass_on(half(left, 0), half(right, 1))
    down_own = halved(down_weight, 0)

    place = jnp.where(my_y == 0, my_z, chips - 1 - my_z)

    def chip_at(by):
        at = (place + by) % chips
        return jnp.where(at < nz, at * ny, (chips - 1 - at) * ny + 1)

    steps = [0]
    for step in range(1, chips // 2):
        steps += [-step, step]
    order = jnp.stack([chip_at(by) for by in (*steps, chips // 2)]).astype(jnp.int32)
    last = 2 * order[-1:]
    up_order = jnp.concatenate([2 * order[:-1], last, last + 1])

    kv_heads = keyvals.shape[1]
    tok_rows = queries.shape[0]
    own_rows = tok_rows // 2
    marked = jnp.concatenate(
        [
            keyvals.reshape(tok_rows, -1),
            jnp.broadcast_to(doc_ids.astype(keyvals.dtype)[:, None], (tok_rows, keyvals.shape[2])),
        ],
        axis=1,
    )
    count = lax.axis_size("sp")
    low = send(marked[-WINDOW_REACH:], [(i, i + 1) for i in range(count - 1)])
    high = send(marked[:WINDOW_REACH], [(i + 1, i) for i in range(count - 1)])
    blocks = own_rows // WINDOW_REACH

    def attended(half):
        place = jnp.stack([half * blocks, me * tok_rows]).astype(jnp.int32)
        return attend_rows(
            kv_heads, count * tok_rows, place, head_sink_logit, queries, low, marked, high, own_rows
        )

    given = attended(1 - tp_me)
    taken = send(given, swap, "tp")
    kept = attended(tp_me)
    joined = jnp.concatenate(
        [jnp.where(tp_me == 0, kept, taken), jnp.where(tp_me == 0, taken, kept)], axis=1
    )
    projected = jnp.dot(joined, out_weight, preferred_element_type=jnp.float32)
    first_stream = layer_norm(stream_in.astype(jnp.float32) + projected, first_gain).astype(
        jnp.bfloat16
    )
    peer_stream = send(first_stream, swap, "tp")
    twin_stream = send(first_stream, twin)
    far_stream = send(peer_stream, twin)
    twin_active, own_active, peer_active = up_project(
        up_order, (twin_stream, far_stream, first_stream, peer_stream), up_blocks
    )

    def after(value, *results):
        return lax.optimization_barrier((value, *results))[0]

    left, right = pass_on(down_own, down_own)
    left, right = after(left, twin_active), after(right, twin_active)
    column_blocks = [down_own]
    mine, theirs = [], []
    for number in range(chips):
        step = (number + 1) // 2
        if number % 2 == 1 and step < chips // 2:
            column_blocks += [left, right]
            if step + 1 < chips // 2:
                left, right = pass_on(left, right)
            else:
                left, right = pass_on(half(left, 0), half(right, 1))
        elif number == chips - 1:
            column_blocks.append(jnp.concatenate([left, right], axis=0))
        weight = column_blocks[number]
        share = jnp.dot(twin_active, weight, preferred_element_type=jnp.float32).astype(
            jnp.bfloat16
        )
        from_twin = send(share, twin).astype(jnp.float32)
        to_peer = (
            jnp.dot(peer_active, weight, preferred_element_type=jnp.float32)
            + from_twin[own_rows:]
        ).astype(jnp.bfloat16)
        theirs.append(send(to_peer, swap, "tp"))
        kept = (
            jnp.dot(own_active, weight, preferred_element_type=jnp.float32)
            + from_twin[:own_rows]
        ).astype(jnp.bfloat16)
        mine.append(kept)
        if number % 2 == 0 and number > 0:
            left, right = after(left, to_peer, kept), after(right, to_peer, kept)
    return norm_sum(order, first_stream, second_gain, mine, theirs)


def solution(mesh):
    shape = line_shape(mesh)
    body = per_device if shape is None else functools.partial(per_device_line, shape)
    return jax.shard_map(
        body,
        mesh=mesh,
        in_specs=(
            P("sp", "tp"),
            P("sp", "tp", None),
            P("tp"),
            P("sp"),
            P(("sp", "tp"), None),
            P(),
            P(),
            P("sp", "tp"),
            P("tp", "sp"),
            P(),
        ),
        out_specs=P(("sp", "tp"), None),
        check_vma=False,
    )
```

```python
import functools

import jax
import jax.numpy as jnp
from jax import lax
from jax.experimental import pallas as pl
from jax.experimental.pallas import tpu as pltpu
from jax.sharding import PartitionSpec as P

HEAD_SIZE = 64
WINDOW_REACH = 128


NEG_LARGE = -1e30
NORM_EPS = 1e-05

VMEM_SMALL = 14 * 2**20
VMEM_LARGE = 58 * 2**20


def padded(block, sides, width):
    for axis, dim in sides:
        count = lax.axis_size(axis)
        forward = [(i, i + 1) for i in range(count - 1)]
        backward = [(target, source) for source, target in forward]
        low = lax.ppermute(
            lax.slice_in_dim(block, block.shape[dim] - width, None, axis=dim), axis, forward
        )
        high = lax.ppermute(lax.slice_in_dim(block, 0, width, axis=dim), axis, backward)
        block = jnp.concatenate([low, block, high], axis=dim)
    return block


def layer_norm(stream, gain_row):
    centre = jnp.mean(stream, axis=-1, keepdims=True)
    shifted = stream - centre
    spread = jnp.mean(shifted * shifted, axis=-1, keepdims=True)
    return shifted * lax.rsqrt(spread + NORM_EPS) * gain_row


def attend(queries, keyvals, head_sink_logit, doc_ids):
    tok_rows = queries.shape[0]
    kv_heads = keyvals.shape[1]
    heads_per_group = queries.shape[1] // (HEAD_SIZE * kv_heads)
    block_list = tok_rows // WINDOW_REACH
    score_scale = HEAD_SIZE ** (-0.5)
    doc_marks = doc_ids.astype(jnp.bfloat16)
    rim_keys, rim_docs = (
        padded(keyvals, (("sp", 0),), WINDOW_REACH),
        padded(doc_marks, (("sp", 0),), WINDOW_REACH),
    )
    padded_rows = rim_keys.reshape(block_list + 2, WINDOW_REACH, kv_heads, 2 * HEAD_SIZE)
    banded = jnp.concatenate([padded_rows[:-2], padded_rows[1:-1], padded_rows[2:]], axis=1)
    doc_ext = rim_docs.reshape(block_list + 2, WINDOW_REACH)
    doc_band = jnp.concatenate([doc_ext[:-2], doc_ext[1:-1], doc_ext[2:]], axis=1)
    offset = lax.axis_index("sp") * tok_rows
    total_rows = tok_rows * lax.axis_size("sp")
    query_pos = offset + jnp.arange(tok_rows, dtype=jnp.int32).reshape(block_list, WINDOW_REACH, 1)
    key_pos = (
        offset
        + (
            jnp.arange(block_list, dtype=jnp.int32)[:, None] * WINDOW_REACH
            + jnp.arange(3 * WINDOW_REACH, dtype=jnp.int32)[None, :]
            - WINDOW_REACH
        )[:, None, :]
    )
    allowed = (
        (jnp.abs(query_pos - key_pos) <= WINDOW_REACH)
        & (key_pos >= 0)
        & (key_pos < total_rows)
        & (doc_marks.reshape(block_list, WINDOW_REACH, 1) == doc_band[:, None, :])
    )
    query_block_list = queries.reshape(
        block_list, WINDOW_REACH, kv_heads, heads_per_group, HEAD_SIZE
    )
    scores = (
        jnp.einsum(
            "nqhgd,nkhd->nhgqk",
            query_block_list,
            banded[..., :HEAD_SIZE],
            preferred_element_type=jnp.float32,
        )
        * score_scale
    )
    scores = jnp.where(allowed[:, None, None], scores, NEG_LARGE)
    sink_col = head_sink_logit.reshape(kv_heads, heads_per_group)[None, :, :, None, None]
    highest = jnp.maximum(jnp.max(scores, axis=-1, keepdims=True), sink_col)
    powers = jnp.exp(scores - highest)
    denominator = jnp.sum(powers, axis=-1, keepdims=True) + jnp.exp(sink_col - highest)
    weights = (powers / denominator).astype(jnp.bfloat16)
    mixed_out = jnp.einsum(
        "nhgqk,nkhd->nqhgd", weights, banded[..., HEAD_SIZE:], preferred_element_type=jnp.float32
    )
    return mixed_out.astype(jnp.bfloat16).reshape(tok_rows, kv_heads * heads_per_group * HEAD_SIZE)


def per_device(
    queries,
    keyvals,
    head_sink_logit,
    doc_ids,
    stream_in,
    out_weight,
    first_gain,
    up_weight,
    down_weight,
    second_gain,
):
    up_whole = lax.all_gather(up_weight, "sp", axis=0, tiled=True)
    down_whole = lax.all_gather(down_weight, "sp", axis=1, tiled=True)
    attended = attend(queries, keyvals, head_sink_logit, doc_ids)
    tp_count = lax.axis_size("tp")
    own_rows = attended.shape[0] // tp_count
    by_peer = attended.reshape(tp_count, own_rows, attended.shape[1])
    projected = jnp.dot(
        lax.all_to_all(by_peer, "tp", split_axis=0, concat_axis=2, tiled=True)[0],
        out_weight,
        preferred_element_type=jnp.float32,
    )[None][0]
    first_stream = layer_norm(stream_in.astype(jnp.float32) + projected, first_gain).astype(
        jnp.bfloat16
    )
    hidden = jnp.dot(
        lax.all_gather(first_stream, "tp", axis=0, tiled=True),
        up_whole,
        preferred_element_type=jnp.float32,
    )
    active = jnp.square(jnp.maximum(hidden, 0.0)).astype(jnp.bfloat16)
    mixed_out = lax.psum_scatter(
        jnp.dot(active, down_whole, preferred_element_type=jnp.float32).astype(jnp.bfloat16),
        "tp",
        scatter_dimension=0,
        tiled=True,
    ).astype(jnp.float32)
    return layer_norm(first_stream.astype(jnp.float32) + mixed_out, second_gain).astype(
        jnp.bfloat16
    )


def attend_body(kv_heads, total_rows, place, sinks, query, low, own, high, out, band, held, probs):
    reach = WINDOW_REACH
    tok_rows = own.shape[0]
    unit = 2 * HEAD_SIZE
    step = pl.program_id(0)
    block = place[0] + step

    @pl.when(step == 0)
    def _():
        band[:reach] = low[...]
        band[reach : reach + tok_rows] = own[...]
        band[reach + tok_rows :] = high[...]

    start = pl.multiple_of(block * reach, reach)
    marks = slice(kv_heads * unit, (kv_heads + 1) * unit)
    key_docs = band[pl.ds(start, 3 * reach), marks].astype(jnp.float32).T
    query_docs = band[pl.ds(start + reach, reach), marks].astype(jnp.float32)
    shape = (reach, 3 * reach)
    row = lax.broadcasted_iota(jnp.int32, shape, 0)
    column = lax.broadcasted_iota(jnp.int32, shape, 1) - reach
    key_pos = place[1] + start + column
    allowed = (
        (jnp.abs(row - column) <= reach)
        & (key_pos >= 0)
        & (key_pos < total_rows)
        & (key_docs[:reach] == jnp.concatenate([query_docs] * 3, axis=1))
    )
    key_lanes = lax.broadcasted_iota(jnp.int32, (2 * reach, unit), 1) < HEAD_SIZE
    scale = jnp.array(HEAD_SIZE**-0.5, query.dtype)
    for head in range(kv_heads):
        pair = band[pl.ds(start, 3 * reach), head * unit : (head + 1) * unit]
        first = query[:, head * unit : (head + 1) * unit] * scale
        second = jnp.concatenate([first[:, HEAD_SIZE:], first[:, :HEAD_SIZE]], axis=1)
        both = jnp.concatenate([first, second], axis=0)
        both = jnp.where(key_lanes, both, jnp.zeros_like(both))
        scores = lax.dot_general(
            both, pair, (((1,), (1,)), ((), ())), preferred_element_type=jnp.float32
        )
        for member in range(2):
            part = scores[member * reach : (member + 1) * reach]
            held[2 * head + member] = jnp.where(allowed, part, NEG_LARGE)
    for number in range(2 * kv_heads):
        scores = held[number]
        sink = sinks[number]
        highest = jnp.maximum(jnp.max(scores, axis=-1, keepdims=True), sink)
        powers = jnp.exp(scores - highest)
        denominator = jnp.sum(powers, axis=-1, keepdims=True) + jnp.exp(sink - highest)
        at = slice((number % 2) * reach, (number % 2 + 1) * reach)
        probs[number // 2, at] = (powers * (1.0 / denominator)).astype(probs.dtype)
    for head in range(kv_heads):
        pair = band[pl.ds(start, 3 * reach), head * unit : (head + 1) * unit]
        mixed = jnp.dot(probs[head], pair, preferred_element_type=jnp.float32)
        first = pltpu.roll(mixed[:reach], HEAD_SIZE, 1)
        joined = jnp.where(key_lanes[:reach], first, mixed[reach:])
        out[:, head * unit : (head + 1) * unit] = joined.astype(out.dtype)


def attend_rows(kv_heads, total_rows, place, sinks, queries, low, own, high, rows):
    reach = WINDOW_REACH
    width = queries.shape[1]
    whole = lambda array: pl.BlockSpec(array.shape, lambda n, place, sinks: (0, 0))
    return pl.pallas_call(
        functools.partial(attend_body, kv_heads, total_rows),
        grid_spec=pltpu.PrefetchScalarGridSpec(
            num_scalar_prefetch=2,
            grid=(rows // reach,),
            in_specs=[
                pl.BlockSpec((reach, width), lambda n, place, sinks: (place[0] + n, 0)),
                whole(low),
                whole(own),
                whole(high),
            ],
            out_specs=pl.BlockSpec((reach, width), lambda n, place, sinks: (n, 0)),
            scratch_shapes=[
                pltpu.VMEM((own.shape[0] + 2 * reach, own.shape[1]), own.dtype),
                pltpu.VMEM((2 * kv_heads, reach, 3 * reach), jnp.float32),
                pltpu.VMEM((kv_heads, 2 * reach, 3 * reach), own.dtype),
            ],
        ),
        out_shape=jax.ShapeDtypeStruct((rows, width), queries.dtype),
        cost_estimate=pl.CostEstimate(
            flops=12 * rows * width * reach * 10, bytes_accessed=rows * width * 8, transcendentals=0
        ),
        compiler_params=pltpu.CompilerParams(vmem_limit_bytes=VMEM_SMALL),
        name="attend_rows",
    )(place, sinks, queries, low, own, high)


def line_shape(mesh):
    devices = mesh.devices
    names = list(mesh.axis_names)
    if names != ["sp", "tp"]:
        return None
    count, tp_count = devices.shape
    where = [(*devices[i, 0].coords, devices[i, 0].core_on_chip) for i in range(count)]
    zs = sorted({w[2] for w in where})
    ys = sorted({w[1] for w in where})
    cores = sorted({w[3] for w in where})
    expected = [(where[0][0], y, z, c) for z in zs for y in ys for c in cores]
    if where != expected or tp_count != 2 or (len(zs), len(ys), len(cores)) != (4, 2, 2):
        return None
    return len(zs), len(ys), len(cores)


def up_body(tile, unit, order, *rest):
    count = order.shape[0]
    rows = rest[:4]
    weights = rest[4 : 4 + count]
    outs = rest[4 + count : 7 + count]
    buffer, sems = rest[7 + count :]
    step = pl.program_id(0)
    steps = pl.num_programs(0)

    def copies(index, slot):
        return [
            pltpu.make_async_copy(
                weight.at[:, pl.ds(pl.multiple_of(index * tile, tile), tile)],
                buffer.at[
                    slot, pl.ds(pl.multiple_of(order[j] * unit, unit), weight.shape[0]), :
                ],
                sems.at[slot, j],
            )
            for j, weight in enumerate(weights)
        ]

    slot = lax.rem(step, 2)

    @pl.when(step == 0)
    def _():
        for copy in copies(step, slot):
            copy.start()

    @pl.when(step + 1 < steps)
    def _():
        for copy in copies(step + 1, 1 - slot):
            copy.start()

    for copy in copies(step, slot):
        copy.wait()
    size = rows[0].shape[0]
    places = ((outs[0], 0), (outs[0], size), (outs[1], 0), (outs[2], 0))
    for part, (out, first) in zip(rows, places):
        hidden = jnp.dot(part[...], buffer[slot], preferred_element_type=jnp.float32)
        out[first : first + size] = jnp.square(jnp.maximum(hidden, 0.0)).astype(out.dtype)


def up_project(order, rows, weights):
    hidden_units = weights[0].shape[1]
    unit = min(weight.shape[0] for weight in weights)
    tile = min(512, hidden_units)
    count, width = rows[0].shape
    dtype = rows[0].dtype
    return pl.pallas_call(
        functools.partial(up_body, tile, unit),
        grid_spec=pltpu.PrefetchScalarGridSpec(
            num_scalar_prefetch=1,
            grid=(hidden_units // tile,),
            in_specs=[pl.BlockSpec((count, width), lambda n, order: (0, 0))] * 4
            + [pl.BlockSpec(memory_space=pl.ANY)] * len(weights),
            out_specs=[
                pl.BlockSpec((size, tile), lambda n, order: (0, n))
                for size in (2 * count, count, count)
            ],
            scratch_shapes=[
                pltpu.VMEM((2, width, tile), dtype),
                pltpu.SemaphoreType.DMA((2, len(weights))),
            ],
        ),
        out_shape=[
            jax.ShapeDtypeStruct((size, hidden_units), dtype) for size in (2 * count, count, count)
        ],
        cost_estimate=pl.CostEstimate(
            flops=8 * count * width * hidden_units,
            bytes_accessed=2 * width * hidden_units,
            transcendentals=0,
        ),
        compiler_params=pltpu.CompilerParams(vmem_limit_bytes=VMEM_LARGE),
        name="up_project",
    )(order, *rows, *weights)


def block_dots(rows, weights):
    width = rows.shape[1]
    if weights[0].shape[0] == width:
        return [jnp.dot(rows[...], w[...], preferred_element_type=jnp.float32) for w in weights]
    total, at = None, 0
    for w in weights:
        part = jnp.dot(
            rows[:, at : at + w.shape[0]], w[...], preferred_element_type=jnp.float32
        )
        total = part if total is None else total + part
        at += w.shape[0]
    return [total]


def share_body(count, rows, *rest):
    out = rest[count]
    at = 0
    for part in block_dots(rows, rest[:count]):
        out[:, at : at + part.shape[1]] = part.astype(out.dtype)
        at += part.shape[1]


def sum_body(count, peer, own, from_peer, from_own, *rest):
    to_peer, kept = rest[count:]
    for rows, extra, out in ((peer, from_peer, to_peer), (own, from_own, kept)):
        at = 0
        for part in block_dots(rows, rest[:count]):
            columns = slice(at, at + part.shape[1])
            out[:, columns] = (part + extra[:, columns].astype(jnp.float32)).astype(out.dtype)
            at += part.shape[1]


def columns_of(rows, weights):
    whole = weights[0].shape[0] == rows.shape[1]
    return weights[0].shape[1] * (len(weights) if whole else 1)


def share_of(rows, weights):
    count, width = rows.shape
    tile = min(512, count)
    columns = columns_of(rows, weights)
    return pl.pallas_call(
        functools.partial(share_body, len(weights)),
        grid=(count // tile,),
        in_specs=[
            pl.BlockSpec((tile, width), lambda n: (n, 0)),
            *(pl.BlockSpec(w.shape, lambda n: (0, 0)) for w in weights),
        ],
        out_specs=pl.BlockSpec((tile, columns), lambda n: (n, 0)),
        out_shape=jax.ShapeDtypeStruct((count, columns), rows.dtype),
        cost_estimate=pl.CostEstimate(
            flops=2 * count * width * columns,
            bytes_accessed=2 * (count + columns) * width,
            transcendentals=0,
        ),
        compiler_params=pltpu.CompilerParams(vmem_limit_bytes=VMEM_SMALL),
        name="share_of",
    )(rows, *weights)


def sum_of(peer, own, from_twin, weights):
    count, width = own.shape
    tile = min(256, count)
    steps = count // tile
    columns = columns_of(own, weights)
    rows = pl.BlockSpec((tile, width), lambda n: (n, 0))
    found = pl.BlockSpec((tile, columns), lambda n: (n, 0))
    return pl.pallas_call(
        functools.partial(sum_body, len(weights)),
        grid=(steps,),
        in_specs=[
            rows,
            rows,
            pl.BlockSpec((tile, columns), lambda n: (n + steps, 0)),
            found,
            *(pl.BlockSpec(w.shape, lambda n: (0, 0)) for w in weights),
        ],
        out_specs=[found, found],
        out_shape=[jax.ShapeDtypeStruct((count, columns), own.dtype)] * 2,
        cost_estimate=pl.CostEstimate(
            flops=4 * count * width * columns,
            bytes_accessed=2 * (2 * count + columns) * width,
            transcendentals=0,
        ),
        compiler_params=pltpu.CompilerParams(vmem_limit_bytes=VMEM_SMALL),
        name="sum_of",
    )(peer, own, from_twin, from_twin, *weights)


def norm_body(parts, order, stream, gain, *rest):
    mine = rest[:parts]
    theirs = rest[parts : 2 * parts]
    out, total = rest[2 * parts :]
    block = 0
    width = total.shape[1]
    unit = width // order.shape[0]
    for own, other in zip(mine, theirs):
        for j in range(own.shape[1] // unit):
            at = pl.ds(pl.multiple_of(order[block] * unit, unit), unit)
            piece = slice(j * unit, (j + 1) * unit)
            total[:, at] = own[:, piece].astype(jnp.float32) + other[:, piece].astype(jnp.float32)
            block += 1
    full = stream[...].astype(jnp.float32) + total[...]
    out[...] = layer_norm(full, gain[...]).astype(out.dtype)


def norm_sum(order, stream, gain, mine, theirs):
    rows, width = stream.shape
    tile = min(128, rows)
    part_specs = [
        pl.BlockSpec((tile, part.shape[1]), lambda n, order: (n, 0)) for part in [*mine, *theirs]
    ]
    return pl.pallas_call(
        functools.partial(norm_body, len(mine)),
        grid_spec=pltpu.PrefetchScalarGridSpec(
            num_scalar_prefetch=1,
            grid=(rows // tile,),
            in_specs=[
                pl.BlockSpec((tile, width), lambda n, order: (n, 0)),
                pl.BlockSpec((1, width), lambda n, order: (0, 0)),
                *part_specs,
            ],
            out_specs=pl.BlockSpec((tile, width), lambda n, order: (n, 0)),
            scratch_shapes=[pltpu.VMEM((tile, width), jnp.float32)],
        ),
        out_shape=jax.ShapeDtypeStruct((rows, width), stream.dtype),
        compiler_params=pltpu.CompilerParams(vmem_limit_bytes=VMEM_SMALL),
        name="norm_sum",
    )(order, stream, gain.reshape(1, width), *mine, *theirs)


def per_device_line(
    shape,
    queries,
    keyvals,
    head_sink_logit,
    doc_ids,
    stream_in,
    out_weight,
    first_gain,
    up_weight,
    down_weight,
    second_gain,
):
    nz, ny, nc = shape

    def index(z, y, c):
        return (z * ny + y) * nc + c

    def pairs(target):
        found = []
        for z in range(nz):
            for y in range(ny):
                for c in range(nc):
                    to = target(z, y, c)
                    if to is not None:
                        found.append((index(z, y, c), index(*to)))
        return found

    ring = [(z, 0) for z in range(nz)] + [(z, 1) for z in reversed(range(nz))]
    chips = len(ring)

    def turned(by):
        return pairs(lambda z, y, c: (*ring[(ring.index((z, y)) + by) % chips], c))

    onward = turned(1)
    backward = turned(-1)
    twin = pairs(lambda z, y, c: (z, y, 1 - c))
    swap = [(0, 1), (1, 0)]

    me = lax.axis_index("sp")
    my_c = me % nc
    my_y = (me // nc) % ny
    my_z = me // (nc * ny)
    tp_me = lax.axis_index("tp")

    def send(value, way, axis="sp"):
        return lax.ppermute(value, axis, way)

    def halved(weight, hidden_axis):
        half = weight.shape[hidden_axis] // nc
        kept = lax.dynamic_slice_in_dim(weight, my_c * half, half, hidden_axis)
        given = lax.dynamic_slice_in_dim(weight, (1 - my_c) * half, half, hidden_axis)
        taken = send(given, twin)
        low = jnp.where(my_c == 0, kept, taken)
        high = jnp.where(my_c == 0, taken, kept)
        return jnp.concatenate([low, high], axis=1 - hidden_axis)

    def pass_on(left, right):
        return send(left, onward), send(right, backward)

    def half(block, number):
        rows = block.shape[0] // 2
        return lax.slice_in_dim(block, number * rows, (number + 1) * rows, axis=0)

    up_own = halved(up_weight, 1)
    up_blocks = [up_own]
    left = right = up_own
    for _ in range(1, chips // 2):
        left, right = pass_on(left, right)
        up_blocks += [left, right]
    up_blocks += pass_on(half(left, 0), half(right, 1))
    down_own = halved(down_weight, 0)

    place = jnp.where(my_y == 0, my_z, chips - 1 - my_z)

    def chip_at(by):
        at = (place + by) % chips
        return jnp.where(at < nz, at * ny, (chips - 1 - at) * ny + 1)

    steps = [0]
    for step in range(1, chips // 2):
        steps += [-step, step]
    order = jnp.stack([chip_at(by) for by in (*steps, chips // 2)]).astype(jnp.int32)
    last = 2 * order[-1:]
    up_order = jnp.concatenate([2 * order[:-1], last, last + 1])

    kv_heads = keyvals.shape[1]
    tok_rows = queries.shape[0]
    own_rows = tok_rows // 2
    marked = jnp.concatenate(
        [
            keyvals.reshape(tok_rows, -1),
            jnp.broadcast_to(doc_ids.astype(keyvals.dtype)[:, None], (tok_rows, keyvals.shape[2])),
        ],
        axis=1,
    )
    count = lax.axis_size("sp")
    low = send(marked[-WINDOW_REACH:], [(i, i + 1) for i in range(count - 1)])
    high = send(marked[:WINDOW_REACH], [(i + 1, i) for i in range(count - 1)])
    blocks = own_rows // WINDOW_REACH

    def attended(half):
        place = jnp.stack([half * blocks, me * tok_rows]).astype(jnp.int32)
        return attend_rows(
            kv_heads, count * tok_rows, place, head_sink_logit, queries, low, marked, high, own_rows
        )

    given = attended(1 - tp_me)
    taken = send(given, swap, "tp")
    kept = attended(tp_me)
    joined = jnp.concatenate(
        [jnp.where(tp_me == 0, kept, taken), jnp.where(tp_me == 0, taken, kept)], axis=1
    )
    projected = jnp.dot(joined, out_weight, preferred_element_type=jnp.float32)
    first_stream = layer_norm(stream_in.astype(jnp.float32) + projected, first_gain).astype(
        jnp.bfloat16
    )
    peer_stream = send(first_stream, swap, "tp")
    twin_stream = send(first_stream, twin)
    far_stream = send(peer_stream, twin)
    twin_active, own_active, peer_active = up_project(
        up_order, (twin_stream, far_stream, first_stream, peer_stream), up_blocks
    )

    def after(value, *results):
        return lax.optimization_barrier((value, *results))[0]

    left, right = pass_on(down_own, down_own)
    left, right = after(left, twin_active), after(right, twin_active)
    mine, theirs = [], []

    def share(weights):
        given = share_of(twin_active, weights)
        return send(given, twin)

    def summed(from_twin, weights):
        to_peer, kept = sum_of(peer_active, own_active, from_twin, weights)
        mine.append(kept)
        theirs.append(send(to_peer, swap, "tp"))
        return to_peer

    from_twin = share((down_own,))
    for step in range(1, chips // 2 + 1):
        pair = (left, right)
        if step + 1 < chips // 2:
            left, right = pass_on(left, right)
        elif step + 1 == chips // 2:
            left, right = pass_on(half(left, 0), half(right, 1))
        from_twin_too = share(pair)
        if step == 1:
            summed(from_twin, (down_own,))
        done = summed(from_twin_too, pair)
        left, right = after(left, done), after(right, done)
    return norm_sum(order, first_stream, second_gain, mine, theirs)


def solution(mesh):
    shape = line_shape(mesh)
    body = per_device if shape is None else functools.partial(per_device_line, shape)
    return jax.shard_map(
        body,
        mesh=mesh,
        in_specs=(
            P("sp", "tp"),
            P("sp", "tp", None),
            P("tp"),
            P("sp"),
            P(("sp", "tp"), None),
            P(),
            P(),
            P("sp", "tp"),
            P("tp", "sp"),
            P(),
        ),
        out_specs=P(("sp", "tp"), None),
        check_vma=False,
    )
```

```python
import functools

import jax
import jax.numpy as jnp
from jax import lax
from jax.experimental import pallas as pl
from jax.experimental.pallas import tpu as pltpu
from jax.sharding import PartitionSpec as P

HEAD_SIZE = 64
WINDOW_REACH = 128


NEG_LARGE = -1e30
NORM_EPS = 1e-05

VMEM_SMALL = 14 * 2**20
VMEM_LARGE = 58 * 2**20


def padded(block, sides, width):
    for axis, dim in sides:
        count = lax.axis_size(axis)
        forward = [(i, i + 1) for i in range(count - 1)]
        backward = [(target, source) for source, target in forward]
        low = lax.ppermute(
            lax.slice_in_dim(block, block.shape[dim] - width, None, axis=dim), axis, forward
        )
        high = lax.ppermute(lax.slice_in_dim(block, 0, width, axis=dim), axis, backward)
        block = jnp.concatenate([low, block, high], axis=dim)
    return block


def layer_norm(stream, gain_row):
    centre = jnp.mean(stream, axis=-1, keepdims=True)
    shifted = stream - centre
    spread = jnp.mean(shifted * shifted, axis=-1, keepdims=True)
    return shifted * lax.rsqrt(spread + NORM_EPS) * gain_row


def attend(queries, keyvals, head_sink_logit, doc_ids):
    tok_rows = queries.shape[0]
    kv_heads = keyvals.shape[1]
    heads_per_group = queries.shape[1] // (HEAD_SIZE * kv_heads)
    block_list = tok_rows // WINDOW_REACH
    score_scale = HEAD_SIZE ** (-0.5)
    doc_marks = doc_ids.astype(jnp.bfloat16)
    rim_keys, rim_docs = (
        padded(keyvals, (("sp", 0),), WINDOW_REACH),
        padded(doc_marks, (("sp", 0),), WINDOW_REACH),
    )
    padded_rows = rim_keys.reshape(block_list + 2, WINDOW_REACH, kv_heads, 2 * HEAD_SIZE)
    banded = jnp.concatenate([padded_rows[:-2], padded_rows[1:-1], padded_rows[2:]], axis=1)
    doc_ext = rim_docs.reshape(block_list + 2, WINDOW_REACH)
    doc_band = jnp.concatenate([doc_ext[:-2], doc_ext[1:-1], doc_ext[2:]], axis=1)
    offset = lax.axis_index("sp") * tok_rows
    total_rows = tok_rows * lax.axis_size("sp")
    query_pos = offset + jnp.arange(tok_rows, dtype=jnp.int32).reshape(block_list, WINDOW_REACH, 1)
    key_pos = (
        offset
        + (
            jnp.arange(block_list, dtype=jnp.int32)[:, None] * WINDOW_REACH
            + jnp.arange(3 * WINDOW_REACH, dtype=jnp.int32)[None, :]
            - WINDOW_REACH
        )[:, None, :]
    )
    allowed = (
        (jnp.abs(query_pos - key_pos) <= WINDOW_REACH)
        & (key_pos >= 0)
        & (key_pos < total_rows)
        & (doc_marks.reshape(block_list, WINDOW_REACH, 1) == doc_band[:, None, :])
    )
    query_block_list = queries.reshape(
        block_list, WINDOW_REACH, kv_heads, heads_per_group, HEAD_SIZE
    )
    scores = (
        jnp.einsum(
            "nqhgd,nkhd->nhgqk",
            query_block_list,
            banded[..., :HEAD_SIZE],
            preferred_element_type=jnp.float32,
        )
        * score_scale
    )
    scores = jnp.where(allowed[:, None, None], scores, NEG_LARGE)
    sink_col = head_sink_logit.reshape(kv_heads, heads_per_group)[None, :, :, None, None]
    highest = jnp.maximum(jnp.max(scores, axis=-1, keepdims=True), sink_col)
    powers = jnp.exp(scores - highest)
    denominator = jnp.sum(powers, axis=-1, keepdims=True) + jnp.exp(sink_col - highest)
    weights = (powers / denominator).astype(jnp.bfloat16)
    mixed_out = jnp.einsum(
        "nhgqk,nkhd->nqhgd", weights, banded[..., HEAD_SIZE:], preferred_element_type=jnp.float32
    )
    return mixed_out.astype(jnp.bfloat16).reshape(tok_rows, kv_heads * heads_per_group * HEAD_SIZE)


def per_device(
    queries,
    keyvals,
    head_sink_logit,
    doc_ids,
    stream_in,
    out_weight,
    first_gain,
    up_weight,
    down_weight,
    second_gain,
):
    up_whole = lax.all_gather(up_weight, "sp", axis=0, tiled=True)
    down_whole = lax.all_gather(down_weight, "sp", axis=1, tiled=True)
    attended = attend(queries, keyvals, head_sink_logit, doc_ids)
    tp_count = lax.axis_size("tp")
    own_rows = attended.shape[0] // tp_count
    by_peer = attended.reshape(tp_count, own_rows, attended.shape[1])
    projected = jnp.dot(
        lax.all_to_all(by_peer, "tp", split_axis=0, concat_axis=2, tiled=True)[0],
        out_weight,
        preferred_element_type=jnp.float32,
    )[None][0]
    first_stream = layer_norm(stream_in.astype(jnp.float32) + projected, first_gain).astype(
        jnp.bfloat16
    )
    hidden = jnp.dot(
        lax.all_gather(first_stream, "tp", axis=0, tiled=True),
        up_whole,
        preferred_element_type=jnp.float32,
    )
    active = jnp.square(jnp.maximum(hidden, 0.0)).astype(jnp.bfloat16)
    mixed_out = lax.psum_scatter(
        jnp.dot(active, down_whole, preferred_element_type=jnp.float32).astype(jnp.bfloat16),
        "tp",
        scatter_dimension=0,
        tiled=True,
    ).astype(jnp.float32)
    return layer_norm(first_stream.astype(jnp.float32) + mixed_out, second_gain).astype(
        jnp.bfloat16
    )


def attend_body(kv_heads, total_rows, place, sinks, query, low, own, high, out, band, held, probs):
    reach = WINDOW_REACH
    tok_rows = own.shape[0]
    unit = 2 * HEAD_SIZE
    step = pl.program_id(0)
    block = place[0] + step

    @pl.when(step == 0)
    def _():
        band[:reach] = low[...]
        band[reach : reach + tok_rows] = own[...]
        band[reach + tok_rows :] = high[...]

    start = pl.multiple_of(block * reach, reach)
    marks = slice(kv_heads * unit, (kv_heads + 1) * unit)
    key_docs = band[pl.ds(start, 3 * reach), marks].astype(jnp.float32).T
    query_docs = band[pl.ds(start + reach, reach), marks].astype(jnp.float32)
    shape = (reach, 3 * reach)
    row = lax.broadcasted_iota(jnp.int32, shape, 0)
    column = lax.broadcasted_iota(jnp.int32, shape, 1) - reach
    key_pos = place[1] + start + column
    allowed = (
        (jnp.abs(row - column) <= reach)
        & (key_pos >= 0)
        & (key_pos < total_rows)
        & (key_docs[:reach] == jnp.concatenate([query_docs] * 3, axis=1))
    )
    key_lanes = lax.broadcasted_iota(jnp.int32, (2 * reach, unit), 1) < HEAD_SIZE
    scale = jnp.array(HEAD_SIZE**-0.5, query.dtype)
    for head in range(kv_heads):
        pair = band[pl.ds(start, 3 * reach), head * unit : (head + 1) * unit]
        first = query[:, head * unit : (head + 1) * unit] * scale
        second = jnp.concatenate([first[:, HEAD_SIZE:], first[:, :HEAD_SIZE]], axis=1)
        both = jnp.concatenate([first, second], axis=0)
        both = jnp.where(key_lanes, both, jnp.zeros_like(both))
        scores = lax.dot_general(
            both, pair, (((1,), (1,)), ((), ())), preferred_element_type=jnp.float32
        )
        for member in range(2):
            part = scores[member * reach : (member + 1) * reach]
            held[2 * head + member] = jnp.where(allowed, part, NEG_LARGE)
    for number in range(2 * kv_heads):
        scores = held[number]
        sink = sinks[number]
        highest = jnp.maximum(jnp.max(scores, axis=-1, keepdims=True), sink)
        powers = jnp.exp(scores - highest)
        denominator = jnp.sum(powers, axis=-1, keepdims=True) + jnp.exp(sink - highest)
        at = slice((number % 2) * reach, (number % 2 + 1) * reach)
        probs[number // 2, at] = (powers * (1.0 / denominator)).astype(probs.dtype)
    for head in range(kv_heads):
        pair = band[pl.ds(start, 3 * reach), head * unit : (head + 1) * unit]
        mixed = jnp.dot(probs[head], pair, preferred_element_type=jnp.float32)
        first = pltpu.roll(mixed[:reach], HEAD_SIZE, 1)
        joined = jnp.where(key_lanes[:reach], first, mixed[reach:])
        out[:, head * unit : (head + 1) * unit] = joined.astype(out.dtype)


def attend_rows(kv_heads, total_rows, place, sinks, queries, low, own, high, rows):
    reach = WINDOW_REACH
    width = queries.shape[1]
    whole = lambda array: pl.BlockSpec(array.shape, lambda n, place, sinks: (0, 0))
    return pl.pallas_call(
        functools.partial(attend_body, kv_heads, total_rows),
        grid_spec=pltpu.PrefetchScalarGridSpec(
            num_scalar_prefetch=2,
            grid=(rows // reach,),
            in_specs=[
                pl.BlockSpec((reach, width), lambda n, place, sinks: (place[0] + n, 0)),
                whole(low),
                whole(own),
                whole(high),
            ],
            out_specs=pl.BlockSpec((reach, width), lambda n, place, sinks: (n, 0)),
            scratch_shapes=[
                pltpu.VMEM((own.shape[0] + 2 * reach, own.shape[1]), own.dtype),
                pltpu.VMEM((2 * kv_heads, reach, 3 * reach), jnp.float32),
                pltpu.VMEM((kv_heads, 2 * reach, 3 * reach), own.dtype),
            ],
        ),
        out_shape=jax.ShapeDtypeStruct((rows, width), queries.dtype),
        cost_estimate=pl.CostEstimate(
            flops=12 * rows * width * reach * 10, bytes_accessed=rows * width * 8, transcendentals=0
        ),
        compiler_params=pltpu.CompilerParams(vmem_limit_bytes=VMEM_SMALL),
        name="attend_rows",
    )(place, sinks, queries, low, own, high)


def line_shape(mesh):
    devices = mesh.devices
    names = list(mesh.axis_names)
    if names != ["sp", "tp"]:
        return None
    count, tp_count = devices.shape
    where = [(*devices[i, 0].coords, devices[i, 0].core_on_chip) for i in range(count)]
    zs = sorted({w[2] for w in where})
    ys = sorted({w[1] for w in where})
    cores = sorted({w[3] for w in where})
    expected = [(where[0][0], y, z, c) for z in zs for y in ys for c in cores]
    if where != expected or tp_count != 2 or (len(zs), len(ys), len(cores)) != (4, 2, 2):
        return None
    return len(zs), len(ys), len(cores)


def up_body(tile, order, *rest):
    count = len(rest) - 7
    rows = rest[:2]
    weights = rest[2 : 2 + count]
    out, picked, buffer, row_sems, sems = rest[2 + count :]
    step = pl.program_id(0)
    steps = pl.num_programs(0)
    unit = weights[0].shape[0]
    size = rows[0].shape[0]

    def copies(index, slot):
        return [
            pltpu.make_async_copy(
                weight.at[:, pl.ds(pl.multiple_of(index * tile, tile), tile)],
                buffer.at[slot, j * unit : (j + 1) * unit, :],
                sems.at[slot, j],
            )
            for j, weight in enumerate(weights)
        ]

    row_copies = pick_copies(order, 0, rows, count, picked, row_sems)
    slot = lax.rem(step, 2)

    @pl.when(step == 0)
    def _():
        for copy in (*row_copies, *copies(step, slot)):
            copy.start()

    @pl.when(step + 1 < steps)
    def _():
        for copy in copies(step + 1, 1 - slot):
            copy.start()

    @pl.when(step == 0)
    def _():
        for copy in row_copies:
            copy.wait()

    for copy in copies(step, slot):
        copy.wait()
    for number in range(2):
        at = slice(number * size, (number + 1) * size)
        out[at] = jnp.dot(picked[at], buffer[slot], preferred_element_type=jnp.float32)


def pick_copies(order, first, rows, count, picked, sems):
    size, width = rows[0].shape
    unit = width // order.shape[0]
    return [
        pltpu.make_async_copy(
            part.at[:, pl.ds(pl.multiple_of(order[first + j] * unit, unit), unit)],
            picked.at[number * size : (number + 1) * size, j * unit : (j + 1) * unit],
            sems.at[number, j],
        )
        for number, part in enumerate(rows)
        for j in range(count)
    ]


def up_partial(order, rows, weights):
    hidden_units = weights[0].shape[1]
    unit = weights[0].shape[0]
    tile = min(512, hidden_units)
    count = rows[0].shape[0]
    depth = unit * len(weights)
    return pl.pallas_call(
        functools.partial(up_body, tile),
        grid_spec=pltpu.PrefetchScalarGridSpec(
            num_scalar_prefetch=1,
            grid=(hidden_units // tile,),
            in_specs=[pl.BlockSpec(memory_space=pl.ANY)] * (2 + len(weights)),
            out_specs=pl.BlockSpec((2 * count, tile), lambda n, order: (0, n)),
            scratch_shapes=[
                pltpu.VMEM((2 * count, depth), rows[0].dtype),
                pltpu.VMEM((2, depth, tile), rows[0].dtype),
                pltpu.SemaphoreType.DMA((2, len(weights))),
                pltpu.SemaphoreType.DMA((2, len(weights))),
            ],
        ),
        out_shape=jax.ShapeDtypeStruct((2 * count, hidden_units), jnp.float32),
        cost_estimate=pl.CostEstimate(
            flops=4 * count * depth * hidden_units,
            bytes_accessed=2 * depth * hidden_units,
            transcendentals=0,
        ),
        compiler_params=pltpu.CompilerParams(vmem_limit_bytes=VMEM_LARGE),
        name="up_partial",
    )(order, *rows, *weights)


def finish_body(first, order, *rest):
    rows = rest[:4]
    near, far = rest[4:6]
    weights = rest[6:-6]
    outs = rest[-6:-3]
    picked, joined, row_sems = rest[-3:]
    unit = rows[0].shape[1] // order.shape[0]
    row_copies = pick_copies(order, first, rows, picked.shape[1] // unit, picked, row_sems)

    @pl.when(pl.program_id(0) == 0)
    def _():
        for copy in row_copies:
            copy.start()

    at = 0
    for weight in weights:
        joined[at : at + weight.shape[0]] = weight[...]
        at += weight.shape[0]

    @pl.when(pl.program_id(0) == 0)
    def _():
        for copy in row_copies:
            copy.wait()

    size = rows[0].shape[0]
    one, two = slice(0, size), slice(size, 2 * size)
    places = ((near, one, outs[0], one), (far, one, outs[0], two))
    places += ((near, two, outs[1], one), (far, two, outs[2], one))
    for number, (partial, source, out, target) in enumerate(places):
        hidden = partial[source] + jnp.dot(
            picked[number * size : (number + 1) * size],
            joined[...],
            preferred_element_type=jnp.float32,
        )
        out[target] = jnp.square(jnp.maximum(hidden, 0.0)).astype(out.dtype)


def up_finish(order, first, rows, near, far, weights):
    count, width = rows[0].shape
    hidden_units = near.shape[1]
    tile = min(512, hidden_units)
    dtype = rows[0].dtype
    depth = sum(weight.shape[0] for weight in weights)
    return pl.pallas_call(
        functools.partial(finish_body, first),
        grid_spec=pltpu.PrefetchScalarGridSpec(
            num_scalar_prefetch=1,
            grid=(hidden_units // tile,),
            in_specs=[
                *[pl.BlockSpec(memory_space=pl.ANY)] * 4,
                *[pl.BlockSpec((2 * count, tile), lambda n, order: (0, n))] * 2,
                *[pl.BlockSpec((w.shape[0], tile), lambda n, order: (0, n)) for w in weights],
            ],
            out_specs=[
                pl.BlockSpec((size, tile), lambda n, order: (0, n))
                for size in (2 * count, count, count)
            ],
            scratch_shapes=[
                pltpu.VMEM((4 * count, depth), dtype),
                pltpu.VMEM((depth, tile), dtype),
                pltpu.SemaphoreType.DMA((4, depth * order.shape[0] // width)),
            ],
        ),
        out_shape=[
            jax.ShapeDtypeStruct((size, hidden_units), dtype) for size in (2 * count, count, count)
        ],
        cost_estimate=pl.CostEstimate(
            flops=8 * count * depth * hidden_units,
            bytes_accessed=24 * count * hidden_units,
            transcendentals=0,
        ),
        compiler_params=pltpu.CompilerParams(vmem_limit_bytes=VMEM_LARGE),
        name="up_finish",
    )(order, *rows, near, far, *weights)


def block_dots(rows, weights):
    width = rows.shape[1]
    if weights[0].shape[0] == width:
        return [jnp.dot(rows[...], w[...], preferred_element_type=jnp.float32) for w in weights]
    total, at = None, 0
    for w in weights:
        part = jnp.dot(
            rows[:, at : at + w.shape[0]], w[...], preferred_element_type=jnp.float32
        )
        total = part if total is None else total + part
        at += w.shape[0]
    return [total]


def share_body(count, rows, *rest):
    out = rest[count]
    at = 0
    for part in block_dots(rows, rest[:count]):
        out[:, at : at + part.shape[1]] = part.astype(out.dtype)
        at += part.shape[1]


def sum_body(count, peer, own, from_peer, from_own, *rest):
    to_peer, kept = rest[count:]
    for rows, extra, out in ((peer, from_peer, to_peer), (own, from_own, kept)):
        at = 0
        for part in block_dots(rows, rest[:count]):
            columns = slice(at, at + part.shape[1])
            out[:, columns] = (part + extra[:, columns].astype(jnp.float32)).astype(out.dtype)
            at += part.shape[1]


def columns_of(rows, weights):
    whole = weights[0].shape[0] == rows.shape[1]
    return weights[0].shape[1] * (len(weights) if whole else 1)


def share_of(rows, weights):
    count, width = rows.shape
    tile = min(512, count)
    columns = columns_of(rows, weights)
    return pl.pallas_call(
        functools.partial(share_body, len(weights)),
        grid=(count // tile,),
        in_specs=[
            pl.BlockSpec((tile, width), lambda n: (n, 0)),
            *(pl.BlockSpec(w.shape, lambda n: (0, 0)) for w in weights),
        ],
        out_specs=pl.BlockSpec((tile, columns), lambda n: (n, 0)),
        out_shape=jax.ShapeDtypeStruct((count, columns), rows.dtype),
        cost_estimate=pl.CostEstimate(
            flops=2 * count * width * columns,
            bytes_accessed=2 * (count + columns) * width,
            transcendentals=0,
        ),
        compiler_params=pltpu.CompilerParams(vmem_limit_bytes=VMEM_SMALL),
        name="share_of",
    )(rows, *weights)


def sum_of(peer, own, from_twin, weights):
    count, width = own.shape
    tile = min(256, count)
    steps = count // tile
    columns = columns_of(own, weights)
    rows = pl.BlockSpec((tile, width), lambda n: (n, 0))
    found = pl.BlockSpec((tile, columns), lambda n: (n, 0))
    return pl.pallas_call(
        functools.partial(sum_body, len(weights)),
        grid=(steps,),
        in_specs=[
            rows,
            rows,
            pl.BlockSpec((tile, columns), lambda n: (n + steps, 0)),
            found,
            *(pl.BlockSpec(w.shape, lambda n: (0, 0)) for w in weights),
        ],
        out_specs=[found, found],
        out_shape=[jax.ShapeDtypeStruct((count, columns), own.dtype)] * 2,
        cost_estimate=pl.CostEstimate(
            flops=4 * count * width * columns,
            bytes_accessed=2 * (2 * count + columns) * width,
            transcendentals=0,
        ),
        compiler_params=pltpu.CompilerParams(vmem_limit_bytes=VMEM_SMALL),
        name="sum_of",
    )(peer, own, from_twin, from_twin, *weights)


def norm_body(parts, order, stream, gain, *rest):
    mine = rest[:parts]
    theirs = rest[parts : 2 * parts]
    out, total = rest[2 * parts :]
    block = 0
    width = total.shape[1]
    unit = width // order.shape[0]
    for own, other in zip(mine, theirs):
        for j in range(own.shape[1] // unit):
            at = pl.ds(pl.multiple_of(order[block] * unit, unit), unit)
            piece = slice(j * unit, (j + 1) * unit)
            total[:, at] = own[:, piece].astype(jnp.float32) + other[:, piece].astype(jnp.float32)
            block += 1
    full = stream[...].astype(jnp.float32) + total[...]
    out[...] = layer_norm(full, gain[...]).astype(out.dtype)


def norm_sum(order, stream, gain, mine, theirs):
    rows, width = stream.shape
    tile = min(128, rows)
    part_specs = [
        pl.BlockSpec((tile, part.shape[1]), lambda n, order: (n, 0)) for part in [*mine, *theirs]
    ]
    return pl.pallas_call(
        functools.partial(norm_body, len(mine)),
        grid_spec=pltpu.PrefetchScalarGridSpec(
            num_scalar_prefetch=1,
            grid=(rows // tile,),
            in_specs=[
                pl.BlockSpec((tile, width), lambda n, order: (n, 0)),
                pl.BlockSpec((1, width), lambda n, order: (0, 0)),
                *part_specs,
            ],
            out_specs=pl.BlockSpec((tile, width), lambda n, order: (n, 0)),
            scratch_shapes=[pltpu.VMEM((tile, width), jnp.float32)],
        ),
        out_shape=jax.ShapeDtypeStruct((rows, width), stream.dtype),
        compiler_params=pltpu.CompilerParams(vmem_limit_bytes=VMEM_SMALL),
        name="norm_sum",
    )(order, stream, gain.reshape(1, width), *mine, *theirs)


def per_device_line(
    shape,
    queries,
    keyvals,
    head_sink_logit,
    doc_ids,
    stream_in,
    out_weight,
    first_gain,
    up_weight,
    down_weight,
    second_gain,
):
    nz, ny, nc = shape

    def index(z, y, c):
        return (z * ny + y) * nc + c

    def pairs(target):
        found = []
        for z in range(nz):
            for y in range(ny):
                for c in range(nc):
                    to = target(z, y, c)
                    if to is not None:
                        found.append((index(z, y, c), index(*to)))
        return found

    ring = [(z, 0) for z in range(nz)] + [(z, 1) for z in reversed(range(nz))]
    chips = len(ring)

    def turned(by):
        return pairs(lambda z, y, c: (*ring[(ring.index((z, y)) + by) % chips], c))

    onward = turned(1)
    backward = turned(-1)
    twin = pairs(lambda z, y, c: (z, y, 1 - c))
    swap = [(0, 1), (1, 0)]

    me = lax.axis_index("sp")
    my_c = me % nc
    my_y = (me // nc) % ny
    my_z = me // (nc * ny)
    tp_me = lax.axis_index("tp")

    def send(value, way, axis="sp"):
        return lax.ppermute(value, axis, way)

    def halved(weight, hidden_axis):
        half = weight.shape[hidden_axis] // nc
        kept = lax.dynamic_slice_in_dim(weight, my_c * half, half, hidden_axis)
        given = lax.dynamic_slice_in_dim(weight, (1 - my_c) * half, half, hidden_axis)
        taken = send(given, twin)
        low = jnp.where(my_c == 0, kept, taken)
        high = jnp.where(my_c == 0, taken, kept)
        return jnp.concatenate([low, high], axis=1 - hidden_axis)

    def pass_on(left, right):
        return send(left, onward), send(right, backward)

    def half(block, number):
        rows = block.shape[0] // 2
        return lax.slice_in_dim(block, number * rows, (number + 1) * rows, axis=0)

    up_own = halved(up_weight, 1)
    up_blocks = [up_own]
    left = right = up_own
    for _ in range(1, chips // 2):
        left, right = pass_on(left, right)
        up_blocks += [left, right]
    early = 2 * (chips // 2 - 2) + 1
    up_late = up_blocks[early:]
    up_last = (left, right)
    down_own = halved(down_weight, 0)

    place = jnp.where(my_y == 0, my_z, chips - 1 - my_z)

    def chip_at(by):
        at = (place + by) % chips
        return jnp.where(at < nz, at * ny, (chips - 1 - at) * ny + 1)

    steps = [0]
    for step in range(1, chips // 2):
        steps += [-step, step]
    order = jnp.stack([chip_at(by) for by in (*steps, chips // 2)]).astype(jnp.int32)

    kv_heads = keyvals.shape[1]
    tok_rows = queries.shape[0]
    own_rows = tok_rows // 2
    marked = jnp.concatenate(
        [
            keyvals.reshape(tok_rows, -1),
            jnp.broadcast_to(doc_ids.astype(keyvals.dtype)[:, None], (tok_rows, keyvals.shape[2])),
        ],
        axis=1,
    )
    count = lax.axis_size("sp")
    low = send(marked[-WINDOW_REACH:], [(i, i + 1) for i in range(count - 1)])
    high = send(marked[:WINDOW_REACH], [(i + 1, i) for i in range(count - 1)])
    blocks = own_rows // WINDOW_REACH

    def attended(half):
        place = jnp.stack([half * blocks, me * tok_rows]).astype(jnp.int32)
        return attend_rows(
            kv_heads, count * tok_rows, place, head_sink_logit, queries, low, marked, high, own_rows
        )

    given = attended(1 - tp_me)
    taken = send(given, swap, "tp")
    kept = attended(tp_me)
    joined = jnp.concatenate(
        [jnp.where(tp_me == 0, kept, taken), jnp.where(tp_me == 0, taken, kept)], axis=1
    )
    projected = jnp.dot(joined, out_weight, preferred_element_type=jnp.float32)
    first_stream = layer_norm(stream_in.astype(jnp.float32) + projected, first_gain).astype(
        jnp.bfloat16
    )
    peer_stream = send(first_stream, swap, "tp")
    twin_stream = send(first_stream, twin)
    far_stream = send(peer_stream, twin)

    def after(value, *results):
        return lax.optimization_barrier((value, *results))[0]

    near = up_partial(order, (twin_stream, first_stream), up_blocks[:early])
    left, right = (after(block, near) for block in up_last)
    up_late += pass_on(half(left, 0), half(right, 1))
    far = up_partial(order, (far_stream, peer_stream), up_blocks[:early])
    twin_active, own_active, peer_active = up_finish(
        order,
        early,
        (twin_stream, far_stream, first_stream, peer_stream),
        near,
        far,
        up_late,
    )

    left, right = pass_on(down_own, down_own)
    mine, theirs = [], []

    def share(weights):
        given = share_of(twin_active, weights)
        return send(given, twin)

    def summed(from_twin, weights):
        to_peer, kept = sum_of(peer_active, own_active, from_twin, weights)
        mine.append(kept)
        theirs.append(send(to_peer, swap, "tp"))
        return to_peer

    from_twin = share((down_own,))
    for step in range(1, chips // 2 + 1):
        pair = (left, right)
        if step + 1 < chips // 2:
            left, right = pass_on(left, right)
        elif step + 1 == chips // 2:
            left, right = pass_on(half(left, 0), half(right, 1))
        from_twin_too = share(pair)
        if step == 1:
            summed(from_twin, (down_own,))
        done = summed(from_twin_too, pair)
        if step > 1:
            left, right = after(left, done), after(right, done)
    return norm_sum(order, first_stream, second_gain, mine, theirs)


def solution(mesh):
    shape = line_shape(mesh)
    body = per_device if shape is None else functools.partial(per_device_line, shape)
    return jax.shard_map(
        body,
        mesh=mesh,
        in_specs=(
            P("sp", "tp"),
            P("sp", "tp", None),
            P("tp"),
            P("sp"),
            P(("sp", "tp"), None),
            P(),
            P(),
            P("sp", "tp"),
            P("tp", "sp"),
            P(),
        ),
        out_specs=P(("sp", "tp"), None),
        check_vma=False,
    )
```
